32 devices in a mesh: grp: 2 (over x), fs: 4 (over z), tp: 4 (over y, core).
Axes of the slice: x: 2, y: 2, z: 4, core: 2. Of those that a mesh axis runs over, the one named last changes fastest.
Arguments:
- stream: bfloat16 [2048, 2048], P(('grp', 'fs'), 'tp'), parts along dimension 0, may hold values from -80 to 80
- mixed: bfloat16 [2048, 2048], P(('grp', 'fs'), 'tp'), parts along dimension 0, may hold values from -6 to 6
- out_weight: bfloat16 [2048, 2048], P('fs', 'tp'), may hold values from -0.125 to 0.125
- norm_gain: bfloat16 [2048], P('tp'), may hold values from 0.099609375 to 1.8984375
- up_weight: bfloat16 [2048, 8192], P('fs', 'tp'), may hold values from -0.125 to 0.125
- down_weight: bfloat16 [8192, 2048], P('tp', 'fs'), may hold values from -0.09375 to 0.09375
Outputs:
- result: bfloat16 [2048, 2048], P(('grp', 'fs'), 'tp'), parts along dimension 0
The draws below stay inside these ranges and needn't reach their ends.
There are 2 independent parts, one for each index of `grp`. The reference program is written for one: setup_inputs(seed, part) draws one part's arguments, and reference() takes and returns one part's arrays. A program takes and returns all parts, laid end to end along the dimension named above; an argument that names none is the same for every part. Nothing has to cross between parts.
All inputs are finite; a program needn't handle non-finite values.
Results may differ from the reference program's by a relative error of at most 0.01.
Values may be sent and summed in bfloat16 or wider, within the bound.
A program may use at most 64 MiB of HBM per device.

```python
import jax
import jax.numpy as jnp
from jax import lax

D = 2048
FF = 8192
TOKENS = 1024


def draw_stream(key, part):
    base_key = jax.random.fold_in(key, 11)
    first, second, third = jax.random.split(base_key, 3)
    position = jnp.arange(D, dtype=jnp.float32) / max(D - 1, 1)
    column_scale = jnp.exp(position * jnp.log(4.0)) * jax.random.uniform(second, (D,), jnp.float32, 0.6, 1.4)
    row_scale = jnp.exp(jax.random.uniform(third, (TOKENS, 1), jnp.float32, jnp.log(0.5), jnp.log(2.0)))
    values = jnp.clip(jax.random.normal(first, (TOKENS, D), jnp.float32), -6.0, 6.0) * row_scale
    return (values * column_scale).astype(jnp.bfloat16)


def strengthened(drawn, key, source, target, parts, factor):
    owner, partner = [(jnp.arange(drawn.shape[dim]) // (drawn.shape[dim] // parts)).reshape([-1 if axis == dim else 1 for axis in range(drawn.ndim)]) for dim in (source, target)]
    chosen = jax.random.permutation(key, parts)[partner]
    strong = (owner == chosen) | (owner == (partner + parts // 2) % parts)
    return jnp.where(strong, factor * drawn, drawn)


def levels(key, extent, cuts, low, largest):
    factor_of = 1.0
    for dim, blocks in cuts:
        heights = jax.random.uniform(jax.random.fold_in(jax.random.fold_in(key, 6), dim), (blocks,), jnp.float32, low / len(cuts), largest / len(cuts))
        factor_of = factor_of * jnp.repeat(jnp.exp(heights), extent[dim] // blocks).reshape((-1,) + (1,) * (len(extent) - 1 - dim))
    return factor_of


def scatter_about(own_key, shape, deviation, limit, pieces=(), kind=jnp.bfloat16):
    entries = jax.random.normal(own_key, shape, jnp.float32) * deviation
    if len(pieces) > 0:
        entries = levels(own_key, shape, pieces, -0.22, 0.18) * entries
    return jnp.clip(entries, min=-limit, max=limit).astype(kind)


def noise_with(rng, extent, scale, bound, pieces, heavy, held_as=jnp.bfloat16):
    array = scale * jax.random.normal(rng, extent, jnp.float32)
    if pieces:
        array = array * levels(rng, extent, pieces, -0.22, 0.18)
    return jnp.clip(strengthened(array, jax.random.fold_in(rng, 3), *heavy), -bound, bound).astype(held_as)


def setup_inputs(seed: int = 0, part: int = 0) -> dict:
    keys = jax.random.split(jax.random.key(seed), 7)
    part_keys = jax.random.split(jax.random.fold_in(keys[6], part), 7)
    stream = draw_stream(jax.random.fold_in(jax.random.fold_in(keys[6], part), 71), part)
    mixed = scatter_about(part_keys[1], (TOKENS, D), 1.0, 6.0, ((0, 4), (1, 4)))
    out_weight = scatter_about(keys[2], (D, D), D ** -0.5, 0.125, ((0, 4), (1, 4)))
    norm_gain = jnp.clip(1.0 + 0.18 * jax.random.normal(keys[3], (D,), jnp.float32), 0.099609375, 1.8984375).astype(jnp.bfloat16)
    up_weight = scatter_about(keys[4], (D, FF), D ** -0.5, 0.125, ((0, 4), (1, 4)))
    down_weight = noise_with(keys[5], (FF, D), FF ** -0.5, 0.09375, ((0, 4), (1, 4)), (0, 1, 4, 2.0))
    return dict(stream=stream, mixed=mixed, out_weight=out_weight, norm_gain=norm_gain, up_weight=up_weight, down_weight=down_weight)


epsilon = 1e-06

def reference(stream, mixed, out_weight, norm_gain, up_weight, down_weight):
    projected = jnp.dot(mixed, out_weight, preferred_element_type=jnp.float32)
    resid = (stream.astype(jnp.float32) + projected).astype(jnp.bfloat16)
    widened = resid.astype(jnp.float32)
    energy = lax.optimization_barrier(jnp.mean(widened * widened, axis=-1, keepdims=True))
    normed = (widened * lax.rsqrt(energy + epsilon) * norm_gain.astype(jnp.float32)).astype(jnp.bfloat16)
    up_values = jnp.dot(normed, up_weight, preferred_element_type=jnp.float32)
    activated = jnp.square(jax.nn.relu(up_values)).astype(jnp.bfloat16)
    branch = jnp.dot(activated, down_weight, preferred_element_type=jnp.float32)
    return (widened + branch).astype(jnp.bfloat16)
```

```python
import jax
import jax.numpy as jnp
from jax import lax
from jax.sharding import PartitionSpec as P

epsilon = 1e-06


def fold_product(left, portion):
    return jnp.dot(left, portion, preferred_element_type=jnp.float32)


def gathered_body(stream, mixed, out_weight, norm_gain, up_weight, down_weight):
    mixed_whole = lax.all_gather(mixed, "tp", axis=1, tiled=True)
    projected = fold_product(mixed_whole, lax.all_gather(out_weight, "fs", axis=0, tiled=True))
    resid = (stream.astype(jnp.float32) + projected).astype(jnp.bfloat16)
    widened = resid.astype(jnp.float32)
    resid_whole, gain_whole = (
        lax.all_gather(resid, "tp", axis=1, tiled=True),
        lax.all_gather(norm_gain, "tp", axis=0, tiled=True),
    )
    stream_wide = resid_whole.astype(jnp.float32)
    energy = jnp.mean(stream_wide * stream_wide, axis=1, keepdims=True)
    normed_whole = (
        stream_wide * lax.rsqrt(energy + epsilon) * gain_whole.astype(jnp.float32)
    ).astype(jnp.bfloat16)
    up_full = lax.all_gather(up_weight, "fs", axis=0, tiled=True)
    up_values = jnp.dot(normed_whole, up_full, preferred_element_type=jnp.float32)
    activated = jnp.square(jax.nn.relu(up_values)).astype(jnp.bfloat16)
    partials = jnp.dot(
        activated,
        lax.all_gather(down_weight, "fs", axis=1, tiled=True),
        preferred_element_type=jnp.float32,
    )
    branch = lax.psum_scatter(partials, "tp", scatter_dimension=1, tiled=True)
    return (widened + branch).astype(jnp.bfloat16)


def spread_body(stream, mixed, out_weight, norm_gain, up_weight, down_weight):
    mixed_whole = lax.all_gather(mixed, "tp", axis=1, tiled=True)
    out_full = lax.all_gather(out_weight, "fs", axis=0, tiled=True)
    up_mine = lax.all_to_all(up_weight, "fs", split_axis=1, concat_axis=0, tiled=True)
    down_mine = lax.all_to_all(down_weight, "fs", split_axis=0, concat_axis=1, tiled=True)
    projected = jnp.dot(mixed_whole, out_full, preferred_element_type=jnp.float32)
    resid = (stream.astype(jnp.float32) + projected).astype(jnp.bfloat16)
    rows = lax.all_gather(resid, "fs", axis=0, tiled=True)
    whole = lax.all_gather(rows, "tp", axis=1, tiled=True).astype(jnp.float32)
    gain = lax.all_gather(norm_gain, "tp", axis=0, tiled=True).astype(jnp.float32)
    energy = jnp.mean(whole * whole, axis=1, keepdims=True)
    normed = (whole * lax.rsqrt(energy + epsilon) * gain).astype(jnp.bfloat16)
    up_values = jnp.dot(normed, up_mine, preferred_element_type=jnp.float32)
    activated = jnp.square(jax.nn.relu(up_values)).astype(jnp.bfloat16)
    partials = jnp.dot(activated, down_mine, preferred_element_type=jnp.float32).astype(jnp.bfloat16)
    columns = lax.psum_scatter(partials, "tp", scatter_dimension=1, tiled=True)
    branch = lax.psum_scatter(columns, "fs", scatter_dimension=0, tiled=True)
    return (resid.astype(jnp.float32) + branch.astype(jnp.float32)).astype(jnp.bfloat16)


def solution(mesh):
    placed = (
        P(("grp", "fs"), "tp"),
        P(("grp", "fs"), "tp"),
        P("fs", "tp"),
        P("tp"),
        P("fs", "tp"),
        P("tp", "fs"),
    )
    fs, tp = mesh.shape["fs"], mesh.shape["tp"]

    def call(stream, mixed, out_weight, norm_gain, up_weight, down_weight):
        width, hidden = up_weight.shape
        tokens = stream.shape[0] // mesh.shape["grp"]
        moved_weights = 2 * width * hidden // tp
        moved_rows = 2 * tokens * width + 2 * width * hidden // (tp * fs)
        body = spread_body if moved_rows < moved_weights else gathered_body
        return sharded(body)(stream, mixed, out_weight, norm_gain, up_weight, down_weight)

    def sharded(body):
        return jax.shard_map(
            body, mesh=mesh, in_specs=placed, out_specs=P(("grp", "fs"), "tp"), check_vma=False
        )

    return call
```

```python
import functools

import jax
import jax.numpy as jnp
from jax import lax
from jax.experimental import pallas as pl
from jax.experimental.pallas import tpu as pltpu
from jax.sharding import PartitionSpec as P

epsilon = 1e-06


def fold_product(left, portion):
    return jnp.dot(left, portion, preferred_element_type=jnp.float32)


def gathered_body(stream, mixed, out_weight, norm_gain, up_weight, down_weight):
    mixed_whole = lax.all_gather(mixed, "tp", axis=1, tiled=True)
    projected = fold_product(mixed_whole, lax.all_gather(out_weight, "fs", axis=0, tiled=True))
    resid = (stream.astype(jnp.float32) + projected).astype(jnp.bfloat16)
    widened = resid.astype(jnp.float32)
    resid_whole, gain_whole = (
        lax.all_gather(resid, "tp", axis=1, tiled=True),
        lax.all_gather(norm_gain, "tp", axis=0, tiled=True),
    )
    stream_wide = resid_whole.astype(jnp.float32)
    energy = jnp.mean(stream_wide * stream_wide, axis=1, keepdims=True)
    normed_whole = (
        stream_wide * lax.rsqrt(energy + epsilon) * gain_whole.astype(jnp.float32)
    ).astype(jnp.bfloat16)
    up_full = lax.all_gather(up_weight, "fs", axis=0, tiled=True)
    up_values = jnp.dot(normed_whole, up_full, preferred_element_type=jnp.float32)
    activated = jnp.square(jax.nn.relu(up_values)).astype(jnp.bfloat16)
    partials = jnp.dot(
        activated,
        lax.all_gather(down_weight, "fs", axis=1, tiled=True),
        preferred_element_type=jnp.float32,
    )
    branch = lax.psum_scatter(partials, "tp", scatter_dimension=1, tiled=True)
    return (widened + branch).astype(jnp.bfloat16)


def spread_body(stream, mixed, out_weight, norm_gain, up_weight, down_weight):
    mixed_whole = lax.all_gather(mixed, "tp", axis=1, tiled=True)
    out_full = lax.all_gather(out_weight, "fs", axis=0, tiled=True)
    up_mine = lax.all_to_all(up_weight, "fs", split_axis=1, concat_axis=0, tiled=True)
    down_mine = lax.all_to_all(down_weight, "fs", split_axis=0, concat_axis=1, tiled=True)
    projected = jnp.dot(mixed_whole, out_full, preferred_element_type=jnp.float32)
    resid = (stream.astype(jnp.float32) + projected).astype(jnp.bfloat16)
    rows = lax.all_gather(resid, "fs", axis=0, tiled=True)
    whole = lax.all_gather(rows, "tp", axis=1, tiled=True).astype(jnp.float32)
    gain = lax.all_gather(norm_gain, "tp", axis=0, tiled=True).astype(jnp.float32)
    energy = jnp.mean(whole * whole, axis=1, keepdims=True)
    normed = (whole * lax.rsqrt(energy + epsilon) * gain).astype(jnp.bfloat16)
    up_values = jnp.dot(normed, up_mine, preferred_element_type=jnp.float32)
    activated = jnp.square(jax.nn.relu(up_values)).astype(jnp.bfloat16)
    partials = jnp.dot(activated, down_mine, preferred_element_type=jnp.float32).astype(jnp.bfloat16)
    columns = lax.psum_scatter(partials, "tp", scatter_dimension=1, tiled=True)
    branch = lax.psum_scatter(columns, "fs", scatter_dimension=0, tiled=True)
    return (resid.astype(jnp.float32) + branch.astype(jnp.float32)).astype(jnp.bfloat16)


MESH = pl.DeviceIdType.MESH


def slot_table(fs):
    table, count = {}, 0
    sizes = dict(
        mixed=3, gain=3, out_z=fs, out_x=fs, up_z=fs, up_x=fs, down_z=fs, down_x=fs,
        rows_z=fs, rows_y=fs, rows_c=fs, rows_d=fs, sum_c=fs, sum_y=fs, sum_z=fs, own=fs,
    )
    for name, size in sizes.items():
        table[name] = count
        count += size
    return table, count


def layer_kernel(
    fs, slots,
    stream_ref, mixed_ref, out_ref, gain_ref, up_ref, down_ref, result_ref,
    mixw, gains, wo, wup, wdn, rows, acts, kept, send_c, got_c, send_y, got_y, send_z, got_z,
    send_sem, recv_sem, local_sem,
):
    f32, bf16 = jnp.float32, jnp.bfloat16
    g, i, j = lax.axis_index("grp"), lax.axis_index("fs"), lax.axis_index("tp")
    y, c = j // 2, j % 2
    jc = y * 2 + (1 - c)
    jy = (1 - y) * 2 + c
    jd = (1 - y) * 2 + (1 - c)
    half, width = wo.shape[2], wo.shape[3]
    order = [s for s in (2, 1, 3) if s < fs] if fs == 4 else list(range(1, fs))

    core, across, diag, twin = (g, i, jc), (g, i, jy), (g, i, jd), (1 - g, i, j)

    def ahead(s):
        return lax.rem(i + s, fs)

    def behind(s):
        return lax.rem(i + fs - s, fs)

    def slice_of(s):
        return (g, ahead(s), j)

    sent = []

    def copy(name, k, src, dst, target):
        n = slots[name] + k
        return pltpu.make_async_remote_copy(
            src_ref=src, dst_ref=dst, send_sem=send_sem.at[n], recv_sem=recv_sem.at[n],
            device_id=target, device_id_type=MESH,
        )

    def send(name, k, src, dst, target):
        made = copy(name, k, src, dst, target)
        made.start()
        sent.append(made)

    def arrive(name, k, dst, target):
        copy(name, k, dst, dst, target).wait_recv()

    barrier = pltpu.get_barrier_semaphore()
    greeted = [core, across, diag, twin] + [slice_of(s) for s in order]
    for device in greeted:
        pl.semaphore_signal(barrier, inc=1, device_id=device, device_id_type=MESH)

    local = []

    def keep(src, dst):
        made = pltpu.make_async_copy(src, dst, local_sem.at[len(local)])
        made.start()
        local.append(made)

    def up_piece(owner, part):
        return up_ref.at[pl.ds(part * half, half), pl.ds(pl.multiple_of(owner * width, width), width)]

    def down_piece(owner, part):
        return down_ref.at[pl.ds(owner * 2 * half + part * half, half), :]

    for part in range(2):
        keep(out_ref.at[pl.ds(part * half, half), :], wo.at[i, part])
        keep(up_piece(i, part), wup.at[i, part])
        keep(down_piece(i, part), wdn.at[i, part])
    keep(mixed_ref, mixw.at[j])
    keep(gain_ref, gains.at[j])
    pl.semaphore_wait(barrier, len(greeted))

    send("mixed", 0, mixed_ref, mixw.at[j], across)
    send("mixed", 1, mixed_ref, mixw.at[j], core)
    for s in order:
        send("out_z", s, out_ref.at[pl.ds(g * half, half), :], wo.at[i, g], slice_of(s))
    send("gain", 0, gain_ref, gains.at[j], across)
    send("gain", 1, gain_ref, gains.at[j], core)
    send("gain", 2, gain_ref, gains.at[j], diag)
    for s in order:
        send("up_z", s, up_piece(ahead(s), g), wup.at[i, g], slice_of(s))

    arrive("mixed", 0, mixw.at[jy], across)
    send("mixed", 2, mixw.at[jy], mixw.at[jy], core)
    for s in order:
        b = behind(s)
        arrive("out_z", s, wo.at[b, g], slice_of(s))
        send("out_x", s, wo.at[b, g], wo.at[b, g], twin)
    arrive("mixed", 1, mixw.at[jc], core)
    arrive("mixed", 2, mixw.at[jd], core)
    for made in local:
        made.wait()

    def whole(ref, k):
        return ref[k].reshape(2 * half, width)

    total = stream_ref[...].astype(f32) + jnp.dot(mixw[i], whole(wo, i), preferred_element_type=f32)
    for s in order:
        b = behind(s)
        arrive("out_x", s, wo.at[b, 1 - g], twin)
        total += jnp.dot(mixw[b], whole(wo, b), preferred_element_type=f32)
    rows[j, i] = total.astype(bf16)

    for s in order:
        send("rows_z", s, rows.at[j, i], rows.at[j, i], slice_of(s))
    send("rows_y", 0, rows.at[j, i], rows.at[j, i], across)
    send("rows_c", 0, rows.at[j, i], rows.at[j, i], core)
    for s in order:
        send("down_z", s, down_piece(ahead(s), g), wdn.at[i, g], slice_of(s))

    for s in order:
        b = behind(s)
        arrive("up_z", s, wup.at[b, g], slice_of(s))
        send("up_x", s, wup.at[b, g], wup.at[b, g], twin)
    arrive("rows_y", 0, rows.at[jy, i], across)
    send("rows_d", 0, rows.at[jy, i], rows.at[jy, i], core)
    for s in order:
        b = behind(s)
        arrive("rows_z", s, rows.at[j, b], slice_of(s))
        send("rows_y", s, rows.at[j, b], rows.at[j, b], across)
        send("rows_c", s, rows.at[j, b], rows.at[j, b], core)
    arrive("gain", 0, gains.at[jy], across)
    arrive("gain", 1, gains.at[jc], core)
    arrive("gain", 2, gains.at[jd], diag)
    for s in order:
        arrive("up_x", s, wup.at[behind(s), 1 - g], twin)

    def hidden(t):
        wide = [rows[k, t].astype(f32) for k in range(rows.shape[0])]
        energy = sum(jnp.sum(w * w, axis=1, keepdims=True) for w in wide)
        scale = lax.rsqrt(energy * (1.0 / (len(wide) * width)) + epsilon)
        up = None
        for k, w in enumerate(wide):
            normed = (w * scale * gains[k].astype(f32)).astype(bf16)
            term = jnp.dot(normed, whole(wup, k), preferred_element_type=f32)
            up = term if up is None else up + term
        return jnp.square(jnp.maximum(up, 0.0)).astype(bf16)

    for s in [0] + order:
        b = behind(s)
        if s > 0:
            arrive("rows_y", s, rows.at[jy, b], across)
            send("rows_d", s, rows.at[jy, b], rows.at[jy, b], core)
        arrive("rows_c", s, rows.at[jc, b], core)
        arrive("rows_d", s, rows.at[jd, b], core)
        acts[b] = hidden(b)

    for s in order:
        b = behind(s)
        arrive("down_z", s, wdn.at[b, g], slice_of(s))
        send("down_x", s, wdn.at[b, g], wdn.at[b, g], twin)
    for s in order:
        arrive("down_x", s, wdn.at[behind(s), 1 - g], twin)

    def share(t, column):
        return jnp.dot(acts[t], whole(wdn, column), preferred_element_type=f32)

    last = order + [0]
    for s in last:
        t = ahead(s)
        send_c[t, 0] = share(t, jc).astype(bf16)
        send_c[t, 1] = share(t, jd).astype(bf16)
        send("sum_c", s, send_c.at[t], got_c.at[t], core)
    for s in last:
        t = ahead(s)
        far = share(t, jy)
        kept[t] = share(t, j)
        arrive("sum_c", s, got_c.at[t], core)
        send_y[t] = (far + got_c[t, 1].astype(f32)).astype(bf16)
        send("sum_y", s, send_y.at[t], got_y.at[t], across)
    for s in order:
        t = ahead(s)
        arrive("sum_y", s, got_y.at[t], across)
        send_z[t] = (kept[t] + got_c[t, 0].astype(f32) + got_y[t].astype(f32)).astype(bf16)
        send("sum_z", s, send_z.at[t], got_z.at[i], slice_of(s))
    arrive("sum_y", 0, got_y.at[i], across)
    branch = kept[i] + got_c[i, 0].astype(f32) + got_y[i].astype(f32)
    for s in order:
        b = behind(s)
        arrive("sum_z", s, got_z.at[b], slice_of(s))
        branch += got_z[b].astype(f32)
    result_ref[...] = (rows[j, i].astype(f32) + branch).astype(bf16)
    for made in sent:
        made.wait_send()


def kernel_body(fs, tp, stream, mixed, out_weight, norm_gain, up_weight, down_weight):
    tokens, width = stream.shape
    half = out_weight.shape[0] // 2
    slots, count = slot_table(fs)
    vmem, anywhere = pl.BlockSpec(memory_space=pltpu.VMEM), pl.BlockSpec(memory_space=pl.ANY)
    weights = pltpu.VMEM((fs, 2, half, width), jnp.bfloat16)
    blocks = pltpu.VMEM((fs, tokens, width), jnp.bfloat16)
    pairs = pltpu.VMEM((fs, 2, tokens, width), jnp.bfloat16)
    return pl.pallas_call(
        functools.partial(layer_kernel, fs, slots),
        out_shape=jax.ShapeDtypeStruct((tokens, width), jnp.bfloat16),
        in_specs=[vmem, vmem, anywhere, vmem, anywhere, anywhere],
        out_specs=vmem,
        scratch_shapes=[
            pltpu.VMEM((tp, tokens, width), jnp.bfloat16),
            pltpu.VMEM((tp, 1, width), jnp.bfloat16),
            weights, weights, weights,
            pltpu.VMEM((tp, fs, tokens, width), jnp.bfloat16),
            blocks,
            pltpu.VMEM((fs, tokens, width), jnp.float32),
            pairs, pairs, blocks, blocks, blocks, blocks,
            pltpu.SemaphoreType.DMA((count,)),
            pltpu.SemaphoreType.DMA((count,)),
            pltpu.SemaphoreType.DMA((8,)),
        ],
        compiler_params=pltpu.CompilerParams(
            collective_id=0, has_side_effects=True, vmem_limit_bytes=56 * 1024 * 1024
        ),
    )(stream, mixed, out_weight, norm_gain.reshape(1, width), up_weight, down_weight)


def solution(mesh):
    placed = (
        P(("grp", "fs"), "tp"),
        P(("grp", "fs"), "tp"),
        P("fs", "tp"),
        P("tp"),
        P("fs", "tp"),
        P("tp", "fs"),
    )
    fs, tp = mesh.shape["fs"], mesh.shape["tp"]

    def call(stream, mixed, out_weight, norm_gain, up_weight, down_weight):
        width, hidden = up_weight.shape
        tokens = stream.shape[0] // mesh.shape["grp"]
        moved_weights = 2 * width * hidden // tp
        moved_rows = 2 * tokens * width + 2 * width * hidden // (tp * fs)
        aligned = fs == tp == 4 and (width // tp) % 256 == 0 and (tokens // fs) % 16 == 0
        aligned = aligned and hidden == tp * width
        body = spread_body if moved_rows < moved_weights else gathered_body
        if aligned and moved_rows < moved_weights:
            body = functools.partial(kernel_body, fs, tp)
        return sharded(body)(stream, mixed, out_weight, norm_gain, up_weight, down_weight)

    def sharded(body):
        return jax.shard_map(
            body, mesh=mesh, in_specs=placed, out_specs=P(("grp", "fs"), "tp"), check_vma=False
        )

    return call
```

```python
import functools

import jax
import jax.numpy as jnp
from jax import lax
from jax.experimental import pallas as pl
from jax.experimental.pallas import tpu as pltpu
from jax.sharding import PartitionSpec as P

epsilon = 1e-06


def fold_product(left, portion):
    return jnp.dot(left, portion, preferred_element_type=jnp.float32)


def gathered_body(stream, mixed, out_weight, norm_gain, up_weight, down_weight):
    mixed_whole = lax.all_gather(mixed, "tp", axis=1, tiled=True)
    projected = fold_product(mixed_whole, lax.all_gather(out_weight, "fs", axis=0, tiled=True))
    resid = (stream.astype(jnp.float32) + projected).astype(jnp.bfloat16)
    widened = resid.astype(jnp.float32)
    resid_whole, gain_whole = (
        lax.all_gather(resid, "tp", axis=1, tiled=True),
        lax.all_gather(norm_gain, "tp", axis=0, tiled=True),
    )
    stream_wide = resid_whole.astype(jnp.float32)
    energy = jnp.mean(stream_wide * stream_wide, axis=1, keepdims=True)
    normed_whole = (
        stream_wide * lax.rsqrt(energy + epsilon) * gain_whole.astype(jnp.float32)
    ).astype(jnp.bfloat16)
    up_full = lax.all_gather(up_weight, "fs", axis=0, tiled=True)
    up_values = jnp.dot(normed_whole, up_full, preferred_element_type=jnp.float32)
    activated = jnp.square(jax.nn.relu(up_values)).astype(jnp.bfloat16)
    partials = jnp.dot(
        activated,
        lax.all_gather(down_weight, "fs", axis=1, tiled=True),
        preferred_element_type=jnp.float32,
    )
    branch = lax.psum_scatter(partials, "tp", scatter_dimension=1, tiled=True)
    return (widened + branch).astype(jnp.bfloat16)


def spread_body(stream, mixed, out_weight, norm_gain, up_weight, down_weight):
    mixed_whole = lax.all_gather(mixed, "tp", axis=1, tiled=True)
    out_full = lax.all_gather(out_weight, "fs", axis=0, tiled=True)
    up_mine = lax.all_to_all(up_weight, "fs", split_axis=1, concat_axis=0, tiled=True)
    down_mine = lax.all_to_all(down_weight, "fs", split_axis=0, concat_axis=1, tiled=True)
    projected = jnp.dot(mixed_whole, out_full, preferred_element_type=jnp.float32)
    resid = (stream.astype(jnp.float32) + projected).astype(jnp.bfloat16)
    rows = lax.all_gather(resid, "fs", axis=0, tiled=True)
    whole = lax.all_gather(rows, "tp", axis=1, tiled=True).astype(jnp.float32)
    gain = lax.all_gather(norm_gain, "tp", axis=0, tiled=True).astype(jnp.float32)
    energy = jnp.mean(whole * whole, axis=1, keepdims=True)
    normed = (whole * lax.rsqrt(energy + epsilon) * gain).astype(jnp.bfloat16)
    up_values = jnp.dot(normed, up_mine, preferred_element_type=jnp.float32)
    activated = jnp.square(jax.nn.relu(up_values)).astype(jnp.bfloat16)
    partials = jnp.dot(activated, down_mine, preferred_element_type=jnp.float32).astype(jnp.bfloat16)
    columns = lax.psum_scatter(partials, "tp", scatter_dimension=1, tiled=True)
    branch = lax.psum_scatter(columns, "fs", scatter_dimension=0, tiled=True)
    return (resid.astype(jnp.float32) + branch.astype(jnp.float32)).astype(jnp.bfloat16)


MESH = pl.DeviceIdType.MESH


def slot_table(fs):
    table, count = {}, 0
    hops = 2 * (fs - 1)
    sizes = dict(
        mixed=3, gain=3, out_z=hops, out_x=hops, up_z=fs, up_x=fs, down_z=fs, down_x=fs,
        rows_z=hops, rows_y=hops + 1, rows_c=hops + 1, rows_d=hops + 1,
        sum_c=fs * fs, sum_y=fs, sum_z=fs,
    )
    for name, size in sizes.items():
        table[name] = count
        count += size
    return table, count


def layer_kernel(
    fs, slots,
    stream_ref, mixed_ref, out_ref, gain_ref, up_ref, down_ref, result_ref,
    mixw, gains, wo, wup, wdn, rows, acts, kept, mine, send_c, got_c, send_y, got_y, send_z, got_z,
    send_sem, recv_sem, local_sem,
):
    f32, bf16 = jnp.float32, jnp.bfloat16
    g, i, j = lax.axis_index("grp"), lax.axis_index("fs"), lax.axis_index("tp")
    y, c = j // 2, j % 2
    jc = y * 2 + (1 - c)
    jy = (1 - y) * 2 + c
    jd = (1 - y) * 2 + (1 - c)
    half, width = wo.shape[2], wo.shape[3]
    order = [s for s in (2, 1, 3) if s < fs] if fs == 4 else list(range(1, fs))

    core, across, diag, twin = (g, i, jc), (g, i, jy), (g, i, jd), (1 - g, i, j)

    def ahead(s):
        return lax.rem(i + s, fs)

    def behind(s):
        return lax.rem(i + fs - s, fs)

    def slice_of(s):
        return (g, ahead(s), j)

    sent = []

    def copy(name, k, src, dst, target):
        n = slots[name] + k
        return pltpu.make_async_remote_copy(
            src_ref=src, dst_ref=dst, send_sem=send_sem.at[n], recv_sem=recv_sem.at[n],
            device_id=target, device_id_type=MESH,
        )

    def send(name, k, src, dst, target, given=None):
        made = copy(name, k, src, dst, target)
        made.start()
        sent.append((made, None) if given is None else ((name, k), given))

    both = jnp.logical_and

    hops = [(side, d) for d in range(1, fs) for side in range(2)]

    def hop(side, d):
        return side * (fs - 1) + d - 1

    def neighbour(side):
        return slice_of(1) if side == 0 else slice_of(fs - 1)

    def onward(side):
        return i < fs - 1 if side == 0 else i > 0

    def start_relay(name, src, dst):
        for side in range(2):
            @pl.when(onward(side))
            def _():
                send(name, hop(side, 1), src, dst, neighbour(side), lambda side=side: onward(side))

    def take_relay(name, side, d, block_of, then):
        has = i >= d if side == 0 else i + d < fs
        b = i - d if side == 0 else i + d

        @pl.when(has)
        def _():
            arrive(name, hop(side, d), block_of(b), neighbour(1 - side))
            if d < fs - 1:
                @pl.when(onward(side))
                def _():
                    send(
                        name, hop(side, d + 1), block_of(b), block_of(b), neighbour(side),
                        lambda: both(has, onward(side)),
                    )
            then(b, hop(side, d), lambda: has)

    def arrive(name, k, dst, target):
        copy(name, k, dst, dst, target).wait_recv()

    barrier = pltpu.get_barrier_semaphore()
    greeted = [core, across, diag, twin] + [slice_of(s) for s in order]
    for device in greeted:
        pl.semaphore_signal(barrier, inc=1, device_id=device, device_id_type=MESH)

    local = []

    def keep(src, dst):
        made = pltpu.make_async_copy(src, dst, local_sem.at[len(local)])
        made.start()
        local.append(made)

    def up_piece(owner, part):
        return up_ref.at[pl.ds(part * half, half), pl.ds(pl.multiple_of(owner * width, width), width)]

    def down_piece(owner, part):
        return down_ref.at[pl.ds(owner * 2 * half + part * half, half), :]

    for part in range(2):
        keep(out_ref.at[pl.ds(part * half, half), :], wo.at[i, part])
        keep(up_piece(i, part), wup.at[i, part])
        keep(down_piece(i, part), wdn.at[i, part])
    keep(mixed_ref, mixw.at[j])
    keep(gain_ref, gains.at[j])
    pl.semaphore_wait(barrier, len(greeted))

    send("mixed", 0, mixed_ref, mixw.at[j], across)
    send("mixed", 1, mixed_ref, mixw.at[j], core)
    start_relay("out_z", out_ref.at[pl.ds(g * half, half), :], wo.at[i, g])
    send("gain", 0, gain_ref, gains.at[j], across)
    send("gain", 1, gain_ref, gains.at[j], core)
    send("gain", 2, gain_ref, gains.at[j], diag)

    def out_block(b):
        return wo.at[b, g]

    def out_cross(b, n, has):
        send("out_x", n, out_block(b), out_block(b), twin, has)

    for side, d in hops:
        if d == fs - 1 and side == 0:
            for s in order:
                send("up_z", s, up_piece(ahead(s), g), wup.at[i, g], slice_of(s))
        take_relay("out_z", side, d, out_block, out_cross)
    arrive("mixed", 0, mixw.at[jy], across)
    send("mixed", 2, mixw.at[jy], mixw.at[jy], core)
    arrive("mixed", 1, mixw.at[jc], core)
    arrive("mixed", 2, mixw.at[jd], core)
    for made in local:
        made.wait()

    def whole(ref, k):
        return ref[k].reshape(2 * half, width)

    for side, d in hops:
        has = i >= d if side == 0 else i + d < fs
        b = i - d if side == 0 else i + d

        @pl.when(has)
        def _():
            arrive("out_x", hop(side, d), wo.at[b, 1 - g], twin)

    total = stream_ref[...].astype(f32)
    for k in range(fs):
        total += jnp.dot(mixw[k], whole(wo, k), preferred_element_type=f32)
    rows[j, i] = total.astype(bf16)

    start_relay("rows_z", rows.at[j, i], rows.at[j, i])
    send("rows_y", 0, rows.at[j, i], rows.at[j, i], across)
    send("rows_c", 0, rows.at[j, i], rows.at[j, i], core)

    for s in order:
        b = behind(s)
        arrive("up_z", s, wup.at[b, g], slice_of(s))
        send("up_x", s, wup.at[b, g], wup.at[b, g], twin)
    arrive("rows_y", 0, rows.at[jy, i], across)
    send("rows_d", 0, rows.at[jy, i], rows.at[jy, i], core)

    def rows_block(b):
        return rows.at[j, b]

    def rows_cross(b, n, has):
        send("rows_y", n + 1, rows_block(b), rows_block(b), across, has)
        send("rows_c", n + 1, rows_block(b), rows_block(b), core, has)

    for side, d in hops:
        if d == fs - 1 and side == 0:
            for s in order:
                send("down_z", s, down_piece(ahead(s), g), wdn.at[i, g], slice_of(s))
        take_relay("rows_z", side, d, rows_block, rows_cross)
    arrive("gain", 0, gains.at[jy], across)
    arrive("gain", 1, gains.at[jc], core)
    arrive("gain", 2, gains.at[jd], diag)
    for s in order:
        arrive("up_x", s, wup.at[behind(s), 1 - g], twin)

    def hidden(t):
        wide = [rows[k, t].astype(f32) for k in range(rows.shape[0])]
        energy = sum(jnp.sum(w * w, axis=1, keepdims=True) for w in wide)
        scale = lax.rsqrt(energy * (1.0 / (len(wide) * width)) + epsilon)
        up = None
        for k, w in enumerate(wide):
            normed = (w * scale * gains[k].astype(f32)).astype(bf16)
            term = jnp.dot(normed, whole(wup, k), preferred_element_type=f32)
            up = term if up is None else up + term
        return jnp.square(jnp.maximum(up, 0.0)).astype(bf16)

    arrive("rows_c", 0, rows.at[jc, i], core)
    arrive("rows_d", 0, rows.at[jd, i], core)
    acts[i] = hidden(i)
    for side, d in hops:
        has = i >= d if side == 0 else i + d < fs
        b = i - d if side == 0 else i + d
        n = hop(side, d) + 1

        @pl.when(has)
        def _():
            arrive("rows_y", n, rows.at[jy, b], across)
            send("rows_d", n, rows.at[jy, b], rows.at[jy, b], core, lambda has=has: has)
            arrive("rows_c", n, rows.at[jc, b], core)
            arrive("rows_d", n, rows.at[jd, b], core)
            acts[b] = hidden(b)

    last = order + [0]

    def column(n, k):
        ck, yk = k % 2, k // 2
        w = whole(wdn, k)

        @pl.when(ck != c)
        def _():
            for s in last:
                t = ahead(s)
                send_c[yk, t] = jnp.dot(acts[t], w, preferred_element_type=f32).astype(bf16)
                send("sum_c", n * fs + s, send_c.at[yk, t], got_c.at[yk, t], core, lambda: ck != c)

        @pl.when(ck == c)
        def _():
            for s in last:
                t = ahead(s)
                part = jnp.dot(acts[t], w, preferred_element_type=f32)
                arrive("sum_c", n * fs + s, got_c.at[yk, t], core)
                kept[t] = part + got_c[yk, t].astype(f32)

                @pl.when(yk != y)
                def _():
                    send_y[t] = kept[t].astype(bf16)
                    send("sum_y", s, send_y.at[t], got_y.at[t], across, lambda: both(ck == c, yk != y))

                @pl.when(yk == y)
                def _():
                    mine[t] = kept[t]

    for n, s in enumerate([0] + order):
        if s > 0:
            arrive("down_z", s, wdn.at[behind(s), g], slice_of(s))
            send("down_x", s, wdn.at[behind(s), g], wdn.at[behind(s), g], twin)
            arrive("down_x", s, wdn.at[behind(s), 1 - g], twin)
        column(n, behind(s))
    for s in order:
        t = ahead(s)
        arrive("sum_y", s, got_y.at[t], across)
        send_z[t] = (mine[t] + got_y[t].astype(f32)).astype(bf16)
        send("sum_z", s, send_z.at[t], got_z.at[i], slice_of(s))
    arrive("sum_y", 0, got_y.at[i], across)
    branch = mine[i] + got_y[i].astype(f32)
    for s in order:
        b = behind(s)
        arrive("sum_z", s, got_z.at[b], slice_of(s))
        branch += got_z[b].astype(f32)
    result_ref[...] = (rows[j, i].astype(f32) + branch).astype(bf16)
    for made, given in sent:
        if given is None:
            made.wait_send()
        else:
            block = wo.at[0, 0] if made[0].startswith("out") else rows.at[0, 0]
            pl.when(given())(copy(*made, block, block, core).wait_send)


def kernel_body(fs, tp, stream, mixed, out_weight, norm_gain, up_weight, down_weight):
    tokens, width = stream.shape
    half = out_weight.shape[0] // 2
    slots, count = slot_table(fs)
    vmem, anywhere = pl.BlockSpec(memory_space=pltpu.VMEM), pl.BlockSpec(memory_space=pl.ANY)
    weights = pltpu.VMEM((fs, 2, half, width), jnp.bfloat16)
    blocks = pltpu.VMEM((fs, tokens, width), jnp.bfloat16)
    columns = pltpu.VMEM((2, fs, tokens, width), jnp.bfloat16)
    sums = pltpu.VMEM((fs, tokens, width), jnp.float32)
    return pl.pallas_call(
        functools.partial(layer_kernel, fs, slots),
        out_shape=jax.ShapeDtypeStruct((tokens, width), jnp.bfloat16),
        in_specs=[vmem, vmem, anywhere, vmem, anywhere, anywhere],
        out_specs=vmem,
        scratch_shapes=[
            pltpu.VMEM((tp, tokens, width), jnp.bfloat16),
            pltpu.VMEM((tp, 1, width), jnp.bfloat16),
            weights, weights, weights,
            pltpu.VMEM((tp, fs, tokens, width), jnp.bfloat16),
            blocks,
            sums, sums,
            columns, columns, blocks, blocks, blocks, blocks,
            pltpu.SemaphoreType.DMA((count,)),
            pltpu.SemaphoreType.DMA((count,)),
            pltpu.SemaphoreType.DMA((8,)),
        ],
        compiler_params=pltpu.CompilerParams(
            collective_id=0, has_side_effects=True, vmem_limit_bytes=56 * 1024 * 1024
        ),
    )(stream, mixed, out_weight, norm_gain.reshape(1, width), up_weight, down_weight)


def solution(mesh):
    placed = (
        P(("grp", "fs"), "tp"),
        P(("grp", "fs"), "tp"),
        P("fs", "tp"),
        P("tp"),
        P("fs", "tp"),
        P("tp", "fs"),
    )
    fs, tp = mesh.shape["fs"], mesh.shape["tp"]

    def call(stream, mixed, out_weight, norm_gain, up_weight, down_weight):
        width, hidden = up_weight.shape
        tokens = stream.shape[0] // mesh.shape["grp"]
        moved_weights = 2 * width * hidden // tp
        moved_rows = 2 * tokens * width + 2 * width * hidden // (tp * fs)
        aligned = fs == tp == 4 and (width // tp) % 256 == 0 and (tokens // fs) % 16 == 0
        aligned = aligned and hidden == tp * width
        body = spread_body if moved_rows < moved_weights else gathered_body
        if aligned and moved_rows < moved_weights:
            body = functools.partial(kernel_body, fs, tp)
        return sharded(body)(stream, mixed, out_weight, norm_gain, up_weight, down_weight)

    def sharded(body):
        return jax.shard_map(
            body, mesh=mesh, in_specs=placed, out_specs=P(("grp", "fs"), "tp"), check_vma=False
        )

    return call
```

```python
import functools

import jax
import jax.numpy as jnp
from jax import lax
from jax.experimental import pallas as pl
from jax.experimental.pallas import tpu as pltpu
from jax.sharding import PartitionSpec as P

epsilon = 1e-06


def fold_product(left, portion):
    return jnp.dot(left, portion, preferred_element_type=jnp.float32)


def gathered_body(stream, mixed, out_weight, norm_gain, up_weight, down_weight):
    mixed_whole = lax.all_gather(mixed, "tp", axis=1, tiled=True)
    projected = fold_product(mixed_whole, lax.all_gather(out_weight, "fs", axis=0, tiled=True))
    resid = (stream.astype(jnp.float32) + projected).astype(jnp.bfloat16)
    widened = resid.astype(jnp.float32)
    resid_whole, gain_whole = (
        lax.all_gather(resid, "tp", axis=1, tiled=True),
        lax.all_gather(norm_gain, "tp", axis=0, tiled=True),
    )
    stream_wide = resid_whole.astype(jnp.float32)
    energy = jnp.mean(stream_wide * stream_wide, axis=1, keepdims=True)
    normed_whole = (
        stream_wide * lax.rsqrt(energy + epsilon) * gain_whole.astype(jnp.float32)
    ).astype(jnp.bfloat16)
    up_full = lax.all_gather(up_weight, "fs", axis=0, tiled=True)
    up_values = jnp.dot(normed_whole, up_full, preferred_element_type=jnp.float32)
    activated = jnp.square(jax.nn.relu(up_values)).astype(jnp.bfloat16)
    partials = jnp.dot(
        activated,
        lax.all_gather(down_weight, "fs", axis=1, tiled=True),
        preferred_element_type=jnp.float32,
    )
    branch = lax.psum_scatter(partials, "tp", scatter_dimension=1, tiled=True)
    return (widened + branch).astype(jnp.bfloat16)


def spread_body(stream, mixed, out_weight, norm_gain, up_weight, down_weight):
    mixed_whole = lax.all_gather(mixed, "tp", axis=1, tiled=True)
    out_full = lax.all_gather(out_weight, "fs", axis=0, tiled=True)
    up_mine = lax.all_to_all(up_weight, "fs", split_axis=1, concat_axis=0, tiled=True)
    down_mine = lax.all_to_all(down_weight, "fs", split_axis=0, concat_axis=1, tiled=True)
    projected = jnp.dot(mixed_whole, out_full, preferred_element_type=jnp.float32)
    resid = (stream.astype(jnp.float32) + projected).astype(jnp.bfloat16)
    rows = lax.all_gather(resid, "fs", axis=0, tiled=True)
    whole = lax.all_gather(rows, "tp", axis=1, tiled=True).astype(jnp.float32)
    gain = lax.all_gather(norm_gain, "tp", axis=0, tiled=True).astype(jnp.float32)
    energy = jnp.mean(whole * whole, axis=1, keepdims=True)
    normed = (whole * lax.rsqrt(energy + epsilon) * gain).astype(jnp.bfloat16)
    up_values = jnp.dot(normed, up_mine, preferred_element_type=jnp.float32)
    activated = jnp.square(jax.nn.relu(up_values)).astype(jnp.bfloat16)
    partials = jnp.dot(activated, down_mine, preferred_element_type=jnp.float32).astype(jnp.bfloat16)
    columns = lax.psum_scatter(partials, "tp", scatter_dimension=1, tiled=True)
    branch = lax.psum_scatter(columns, "fs", scatter_dimension=0, tiled=True)
    return (resid.astype(jnp.float32) + branch.astype(jnp.float32)).astype(jnp.bfloat16)


MESH = pl.DeviceIdType.MESH


def slot_table(fs):
    table, count = {}, 0
    hops = 2 * (fs - 1)
    sizes = dict(
        mixed=3, gain=3, out_z=hops, out_x=hops, up_z=fs, up_x=fs, down_z=fs, down_x=fs,
        rows_z=hops, rows_y=hops + 1, rows_c=hops + 1, rows_d=hops + 1,
        sum_c=fs * fs, sum_y=fs, sum_z=fs,
    )
    for name, size in sizes.items():
        table[name] = count
        count += size
    return table, count


def layer_kernel(
    fs, slots,
    stream_ref, mixed_ref, out_ref, gain_ref, up_ref, down_ref, result_ref,
    mixw, gains, wo, wup, wdn, rows, acts, kept, mine, send_c, got_c, send_y, got_y, send_z, got_z,
    send_sem, recv_sem, local_sem,
):
    f32, bf16 = jnp.float32, jnp.bfloat16
    g, i, j = lax.axis_index("grp"), lax.axis_index("fs"), lax.axis_index("tp")
    y, c = j // 2, j % 2
    jc = y * 2 + (1 - c)
    jy = (1 - y) * 2 + c
    jd = (1 - y) * 2 + (1 - c)
    half, width = wo.shape[2], wo.shape[3]
    order = [s for s in (2, 1, 3) if s < fs] if fs == 4 else list(range(1, fs))

    core, across, diag, twin = (g, i, jc), (g, i, jy), (g, i, jd), (1 - g, i, j)

    def ahead(s):
        return lax.rem(i + s, fs)

    def behind(s):
        return lax.rem(i + fs - s, fs)

    def slice_of(s):
        return (g, ahead(s), j)

    sent = []

    def copy(name, k, src, dst, target):
        n = slots[name] + k
        return pltpu.make_async_remote_copy(
            src_ref=src, dst_ref=dst, send_sem=send_sem.at[n], recv_sem=recv_sem.at[n],
            device_id=target, device_id_type=MESH,
        )

    def send(name, k, src, dst, target, given=None):
        made = copy(name, k, src, dst, target)
        made.start()
        sent.append((made, None) if given is None else ((name, k), given))

    both = jnp.logical_and

    hops = [(side, d) for d in range(1, fs) for side in range(2)]

    def hop(side, d):
        return side * (fs - 1) + d - 1

    def neighbour(side):
        return slice_of(1) if side == 0 else slice_of(fs - 1)

    def onward(side):
        return i < fs - 1 if side == 0 else i > 0

    def start_relay(name, src, dst):
        for side in range(2):
            @pl.when(onward(side))
            def _():
                send(name, hop(side, 1), src, dst, neighbour(side), lambda side=side: onward(side))

    def take_relay(name, side, d, block_of, then):
        has = i >= d if side == 0 else i + d < fs
        b = i - d if side == 0 else i + d

        @pl.when(has)
        def _():
            arrive(name, hop(side, d), block_of(b), neighbour(1 - side))
            if d < fs - 1:
                @pl.when(onward(side))
                def _():
                    send(
                        name, hop(side, d + 1), block_of(b), block_of(b), neighbour(side),
                        lambda: both(has, onward(side)),
                    )
            then(b, hop(side, d), lambda: has)

    def arrive(name, k, dst, target):
        copy(name, k, dst, dst, target).wait_recv()

    barrier = pltpu.get_barrier_semaphore()
    greeted = [core, across, diag, twin] + [slice_of(s) for s in order]
    for device in greeted:
        pl.semaphore_signal(barrier, inc=1, device_id=device, device_id_type=MESH)

    local = []

    def keep(src, dst):
        made = pltpu.make_async_copy(src, dst, local_sem.at[len(local)])
        made.start()
        local.append(made)

    def up_piece(owner, part):
        return up_ref.at[pl.ds(part * half, half), pl.ds(pl.multiple_of(owner * width, width), width)]

    def down_piece(owner, part):
        return down_ref.at[pl.ds(owner * 2 * half + part * half, half), :]

    for part in range(2):
        keep(out_ref.at[pl.ds(part * half, half), :], wo.at[i, part])
        keep(up_piece(i, part), wup.at[i, part])
        keep(down_piece(i, part), wdn.at[i, part])
    keep(mixed_ref, mixw.at[j])
    keep(gain_ref, gains.at[j])
    pl.semaphore_wait(barrier, len(greeted))

    send("mixed", 0, mixed_ref, mixw.at[j], across)
    send("mixed", 1, mixed_ref, mixw.at[j], core)
    start_relay("out_z", out_ref.at[pl.ds(g * half, half), :], wo.at[i, g])
    send("gain", 0, gain_ref, gains.at[j], across)
    send("gain", 1, gain_ref, gains.at[j], core)
    send("gain", 2, gain_ref, gains.at[j], diag)

    def out_block(b):
        return wo.at[b, g]

    def out_cross(b, n, has):
        send("out_x", n, out_block(b), out_block(b), twin, has)

    for side, d in hops:
        if d == fs - 1 and side == 0:
            for s in order:
                send("up_z", s, up_piece(ahead(s), g), wup.at[i, g], slice_of(s))
        take_relay("out_z", side, d, out_block, out_cross)
    arrive("mixed", 0, mixw.at[jy], across)
    send("mixed", 2, mixw.at[jy], mixw.at[jy], core)
    arrive("mixed", 1, mixw.at[jc], core)
    arrive("mixed", 2, mixw.at[jd], core)
    for made in local:
        made.wait()

    def whole(ref, k):
        return ref[k].reshape(2 * half, width)

    for side, d in hops:
        has = i >= d if side == 0 else i + d < fs
        b = i - d if side == 0 else i + d

        @pl.when(has)
        def _():
            arrive("out_x", hop(side, d), wo.at[b, 1 - g], twin)

    total = stream_ref[...].astype(f32)
    for k in range(fs):
        total += jnp.dot(mixw[k], whole(wo, k), preferred_element_type=f32)
    rows[j, i] = total.astype(bf16)

    start_relay("rows_z", rows.at[j, i], rows.at[j, i])
    send("rows_y", 0, rows.at[j, i], rows.at[j, i], across)
    send("rows_c", 0, rows.at[j, i], rows.at[j, i], core)

    for s in order:
        b = behind(s)
        arrive("up_z", s, wup.at[b, g], slice_of(s))
        send("up_x", s, wup.at[b, g], wup.at[b, g], twin)
    arrive("rows_y", 0, rows.at[jy, i], across)
    send("rows_d", 0, rows.at[jy, i], rows.at[jy, i], core)

    def rows_block(b):
        return rows.at[j, b]

    def rows_cross(b, n, has):
        send("rows_y", n + 1, rows_block(b), rows_block(b), across, has)
        send("rows_c", n + 1, rows_block(b), rows_block(b), core, has)

    for side, d in hops:
        if d == fs - 1 and side == 0:
            for s in order:
                send("down_z", s, down_piece(ahead(s), g), wdn.at[i, g], slice_of(s))
        take_relay("rows_z", side, d, rows_block, rows_cross)
    arrive("gain", 0, gains.at[jy], across)
    arrive("gain", 1, gains.at[jc], core)
    arrive("gain", 2, gains.at[jd], diag)
    for s in order:
        arrive("up_x", s, wup.at[behind(s), 1 - g], twin)

    def hidden(t):
        wide = [rows[k, t].astype(f32) for k in range(rows.shape[0])]
        energy = sum(jnp.sum(w * w, axis=1, keepdims=True) for w in wide)
        scale = lax.rsqrt(energy * (1.0 / (len(wide) * width)) + epsilon)
        up = None
        for k, w in enumerate(wide):
            normed = (w * scale * gains[k].astype(f32)).astype(bf16)
            term = jnp.dot(normed, whole(wup, k), preferred_element_type=f32)
            up = term if up is None else up + term
        return jnp.square(jnp.maximum(up, 0.0)).astype(bf16)

    def cross_down(s):
        arrive("down_z", s, wdn.at[behind(s), g], slice_of(s))
        send("down_x", s, wdn.at[behind(s), g], wdn.at[behind(s), g], twin)

    arrive("rows_c", 0, rows.at[jc, i], core)
    arrive("rows_d", 0, rows.at[jd, i], core)
    acts[i] = hidden(i)
    for side, d in hops:
        has = i >= d if side == 0 else i + d < fs
        b = i - d if side == 0 else i + d
        n = hop(side, d) + 1
        if d == fs - 1 and side == 0:
            cross_down(order[0])

        @pl.when(has)
        def _():
            arrive("rows_y", n, rows.at[jy, b], across)
            send("rows_d", n, rows.at[jy, b], rows.at[jy, b], core, lambda has=has: has)
            arrive("rows_c", n, rows.at[jc, b], core)
            arrive("rows_d", n, rows.at[jd, b], core)
            acts[b] = hidden(b)

    last = order + [0]

    def column(n, k):
        ck, yk = k % 2, k // 2
        w = whole(wdn, k)

        @pl.when(ck != c)
        def _():
            for s in last:
                t = ahead(s)
                send_c[yk, t] = jnp.dot(acts[t], w, preferred_element_type=f32).astype(bf16)
                send("sum_c", n * fs + s, send_c.at[yk, t], got_c.at[yk, t], core, lambda: ck != c)

        @pl.when(ck == c)
        def _():
            for s in last:
                t = ahead(s)
                part = jnp.dot(acts[t], w, preferred_element_type=f32)
                arrive("sum_c", n * fs + s, got_c.at[yk, t], core)
                kept[t] = part + got_c[yk, t].astype(f32)

                @pl.when(yk != y)
                def _():
                    send_y[t] = kept[t].astype(bf16)
                    send("sum_y", s, send_y.at[t], got_y.at[t], across, lambda: both(ck == c, yk != y))

                @pl.when(yk == y)
                def _():
                    mine[t] = kept[t]

    def owned(given):
        @pl.when(given)
        def _():
            for s in order:
                t = ahead(s)
                arrive("sum_y", s, got_y.at[t], across)
                send_z[t] = (mine[t] + got_y[t].astype(f32)).astype(bf16)
                send("sum_z", s, send_z.at[t], got_z.at[i], slice_of(s), lambda: given)

    early = jnp.logical_or(behind(0) == j, behind(order[0]) == j)
    for n, s in enumerate([0] + order):
        if 0 < n < len(order):
            cross_down(order[n])
        if s > 0:
            arrive("down_x", s, wdn.at[behind(s), 1 - g], twin)
        column(n, behind(s))
        if n == len(order) - 1:
            owned(early)
    owned(jnp.logical_not(early))
    arrive("sum_y", 0, got_y.at[i], across)
    branch = mine[i] + got_y[i].astype(f32)
    for s in order:
        b = behind(s)
        arrive("sum_z", s, got_z.at[b], slice_of(s))
        branch += got_z[b].astype(f32)
    result_ref[...] = (rows[j, i].astype(f32) + branch).astype(bf16)
    for made, given in sent:
        if given is None:
            made.wait_send()
        else:
            block = wo.at[0, 0] if made[0].startswith("out") else rows.at[0, 0]
            pl.when(given())(copy(*made, block, block, core).wait_send)


def kernel_body(fs, tp, stream, mixed, out_weight, norm_gain, up_weight, down_weight):
    tokens, width = stream.shape
    half = out_weight.shape[0] // 2
    slots, count = slot_table(fs)
    vmem, anywhere = pl.BlockSpec(memory_space=pltpu.VMEM), pl.BlockSpec(memory_space=pl.ANY)
    weights = pltpu.VMEM((fs, 2, half, width), jnp.bfloat16)
    blocks = pltpu.VMEM((fs, tokens, width), jnp.bfloat16)
    columns = pltpu.VMEM((2, fs, tokens, width), jnp.bfloat16)
    sums = pltpu.VMEM((fs, tokens, width), jnp.float32)
    return pl.pallas_call(
        functools.partial(layer_kernel, fs, slots),
        out_shape=jax.ShapeDtypeStruct((tokens, width), jnp.bfloat16),
        in_specs=[vmem, vmem, anywhere, vmem, anywhere, anywhere],
        out_specs=vmem,
        scratch_shapes=[
            pltpu.VMEM((tp, tokens, width), jnp.bfloat16),
            pltpu.VMEM((tp, 1, width), jnp.bfloat16),
            weights, weights, weights,
            pltpu.VMEM((tp, fs, tokens, width), jnp.bfloat16),
            blocks,
            sums, sums,
            columns, columns, blocks, blocks, blocks, blocks,
            pltpu.SemaphoreType.DMA((count,)),
            pltpu.SemaphoreType.DMA((count,)),
            pltpu.SemaphoreType.DMA((8,)),
        ],
        compiler_params=pltpu.CompilerParams(
            collective_id=0, has_side_effects=True, vmem_limit_bytes=56 * 1024 * 1024
        ),
    )(stream, mixed, out_weight, norm_gain.reshape(1, width), up_weight, down_weight)


def solution(mesh):
    placed = (
        P(("grp", "fs"), "tp"),
        P(("grp", "fs"), "tp"),
        P("fs", "tp"),
        P("tp"),
        P("fs", "tp"),
        P("tp", "fs"),
    )
    fs, tp = mesh.shape["fs"], mesh.shape["tp"]

    def call(stream, mixed, out_weight, norm_gain, up_weight, down_weight):
        width, hidden = up_weight.shape
        tokens = stream.shape[0] // mesh.shape["grp"]
        moved_weights = 2 * width * hidden // tp
        moved_rows = 2 * tokens * width + 2 * width * hidden // (tp * fs)
        aligned = fs == tp == 4 and (width // tp) % 256 == 0 and (tokens // fs) % 16 == 0
        aligned = aligned and hidden == tp * width
        body = spread_body if moved_rows < moved_weights else gathered_body
        if aligned and moved_rows < moved_weights:
            body = functools.partial(kernel_body, fs, tp)
        return sharded(body)(stream, mixed, out_weight, norm_gain, up_weight, down_weight)

    def sharded(body):
        return jax.shard_map(
            body, mesh=mesh, in_specs=placed, out_specs=P(("grp", "fs"), "tp"), check_vma=False
        )

    return call
```

```python
import functools

import jax
import jax.numpy as jnp
from jax import lax
from jax.experimental import pallas as pl
from jax.experimental.pallas import tpu as pltpu
from jax.sharding import PartitionSpec as P

epsilon = 1e-06


def fold_product(left, portion):
    return jnp.dot(left, portion, preferred_element_type=jnp.float32)


def gathered_body(stream, mixed, out_weight, norm_gain, up_weight, down_weight):
    mixed_whole = lax.all_gather(mixed, "tp", axis=1, tiled=True)
    projected = fold_product(mixed_whole, lax.all_gather(out_weight, "fs", axis=0, tiled=True))
    resid = (stream.astype(jnp.float32) + projected).astype(jnp.bfloat16)
    widened = resid.astype(jnp.float32)
    resid_whole, gain_whole = (
        lax.all_gather(resid, "tp", axis=1, tiled=True),
        lax.all_gather(norm_gain, "tp", axis=0, tiled=True),
    )
    stream_wide = resid_whole.astype(jnp.float32)
    energy = jnp.mean(stream_wide * stream_wide, axis=1, keepdims=True)
    normed_whole = (
        stream_wide * lax.rsqrt(energy + epsilon) * gain_whole.astype(jnp.float32)
    ).astype(jnp.bfloat16)
    up_full = lax.all_gather(up_weight, "fs", axis=0, tiled=True)
    up_values = jnp.dot(normed_whole, up_full, preferred_element_type=jnp.float32)
    activated = jnp.square(jax.nn.relu(up_values)).astype(jnp.bfloat16)
    partials = jnp.dot(
        activated,
        lax.all_gather(down_weight, "fs", axis=1, tiled=True),
        preferred_element_type=jnp.float32,
    )
    branch = lax.psum_scatter(partials, "tp", scatter_dimension=1, tiled=True)
    return (widened + branch).astype(jnp.bfloat16)


def spread_body(stream, mixed, out_weight, norm_gain, up_weight, down_weight):
    mixed_whole = lax.all_gather(mixed, "tp", axis=1, tiled=True)
    out_full = lax.all_gather(out_weight, "fs", axis=0, tiled=True)
    up_mine = lax.all_to_all(up_weight, "fs", split_axis=1, concat_axis=0, tiled=True)
    down_mine = lax.all_to_all(down_weight, "fs", split_axis=0, concat_axis=1, tiled=True)
    projected = jnp.dot(mixed_whole, out_full, preferred_element_type=jnp.float32)
    resid = (stream.astype(jnp.float32) + projected).astype(jnp.bfloat16)
    rows = lax.all_gather(resid, "fs", axis=0, tiled=True)
    whole = lax.all_gather(rows, "tp", axis=1, tiled=True).astype(jnp.float32)
    gain = lax.all_gather(norm_gain, "tp", axis=0, tiled=True).astype(jnp.float32)
    energy = jnp.mean(whole * whole, axis=1, keepdims=True)
    normed = (whole * lax.rsqrt(energy + epsilon) * gain).astype(jnp.bfloat16)
    up_values = jnp.dot(normed, up_mine, preferred_element_type=jnp.float32)
    activated = jnp.square(jax.nn.relu(up_values)).astype(jnp.bfloat16)
    partials = jnp.dot(activated, down_mine, preferred_element_type=jnp.float32).astype(jnp.bfloat16)
    columns = lax.psum_scatter(partials, "tp", scatter_dimension=1, tiled=True)
    branch = lax.psum_scatter(columns, "fs", scatter_dimension=0, tiled=True)
    return (resid.astype(jnp.float32) + branch.astype(jnp.float32)).astype(jnp.bfloat16)


MESH = pl.DeviceIdType.MESH


def slot_table(fs):
    table, count = {}, 0
    hops = 2 * (fs - 1)
    sizes = dict(
        mixed=3, gain=3, out_z=hops, out_x=hops, up_z=fs, up_x=fs, down_z=fs, down_x=fs,
        rows_z=hops, rows_y=hops + 1, rows_c=hops + 1, rows_d=hops + 1,
        sum_c=fs * fs, sum_y=fs, sum_z=fs,
    )
    for name, size in sizes.items():
        table[name] = count
        count += size
    return table, count


def layer_kernel(
    fs, slots,
    stream_ref, mixed_ref, out_ref, gain_ref, up_ref, down_ref, result_ref,
    mixw, gains, wo, wup, wdn, rows, acts, kept, mine, send_c, got_c, send_y, got_y, send_z, got_z,
    send_sem, recv_sem, local_sem,
):
    f32, bf16 = jnp.float32, jnp.bfloat16
    g, i, j = lax.axis_index("grp"), lax.axis_index("fs"), lax.axis_index("tp")
    y, c = j // 2, j % 2
    jc = y * 2 + (1 - c)
    jy = (1 - y) * 2 + c
    jd = (1 - y) * 2 + (1 - c)
    half, width = wo.shape[2], wo.shape[3]
    order = [s for s in (2, 1, 3) if s < fs] if fs == 4 else list(range(1, fs))

    core, across, diag, twin = (g, i, jc), (g, i, jy), (g, i, jd), (1 - g, i, j)

    def ahead(s):
        return lax.rem(i + s, fs)

    def behind(s):
        return lax.rem(i + fs - s, fs)

    def slice_of(s):
        return (g, ahead(s), j)

    sent = []

    def copy(name, k, src, dst, target):
        n = slots[name] + k
        return pltpu.make_async_remote_copy(
            src_ref=src, dst_ref=dst, send_sem=send_sem.at[n], recv_sem=recv_sem.at[n],
            device_id=target, device_id_type=MESH,
        )

    def send(name, k, src, dst, target, given=None):
        made = copy(name, k, src, dst, target)
        made.start()
        sent.append((made, None) if given is None else ((name, k), given))

    both = jnp.logical_and

    hops = [(side, d) for d in range(1, fs) for side in range(2)]

    def hop(side, d):
        return side * (fs - 1) + d - 1

    def neighbour(side):
        return slice_of(1) if side == 0 else slice_of(fs - 1)

    def onward(side):
        return i < fs - 1 if side == 0 else i > 0

    def start_relay(name, src, dst):
        for side in range(2):
            @pl.when(onward(side))
            def _():
                send(name, hop(side, 1), src, dst, neighbour(side), lambda side=side: onward(side))

    def take_relay(name, side, d, block_of, then):
        has = i >= d if side == 0 else i + d < fs
        b = i - d if side == 0 else i + d

        @pl.when(has)
        def _():
            arrive(name, hop(side, d), block_of(b), neighbour(1 - side))
            if d < fs - 1:
                @pl.when(onward(side))
                def _():
                    send(
                        name, hop(side, d + 1), block_of(b), block_of(b), neighbour(side),
                        lambda: both(has, onward(side)),
                    )
            then(b, hop(side, d), lambda: has)

    def arrive(name, k, dst, target):
        copy(name, k, dst, dst, target).wait_recv()

    barrier = pltpu.get_barrier_semaphore()
    greeted = [core, across, diag, twin] + [slice_of(s) for s in order]
    for device in greeted:
        pl.semaphore_signal(barrier, inc=1, device_id=device, device_id_type=MESH)

    local = []

    def keep(src, dst):
        made = pltpu.make_async_copy(src, dst, local_sem.at[len(local)])
        made.start()
        local.append(made)

    def up_piece(owner, part):
        return up_ref.at[pl.ds(part * half, half), pl.ds(pl.multiple_of(owner * width, width), width)]

    def down_piece(owner, part):
        return down_ref.at[pl.ds(owner * 2 * half + part * half, half), :]

    for part in range(2):
        keep(out_ref.at[pl.ds(part * half, half), :], wo.at[i, part])
        keep(up_piece(i, part), wup.at[i, part])
        keep(down_piece(i, part), wdn.at[i, part])
    keep(mixed_ref, mixw.at[j])
    keep(gain_ref, gains.at[j])
    pl.semaphore_wait(barrier, len(greeted))

    send("mixed", 0, mixed_ref, mixw.at[j], across)
    send("mixed", 1, mixed_ref, mixw.at[j], core)
    start_relay("out_z", out_ref.at[pl.ds(g * half, half), :], wo.at[i, g])
    send("gain", 0, gain_ref, gains.at[j], across)
    send("gain", 1, gain_ref, gains.at[j], core)
    send("gain", 2, gain_ref, gains.at[j], diag)

    def out_block(b):
        return wo.at[b, g]

    def out_cross(b, n, has):
        send("out_x", n, out_block(b), out_block(b), twin, has)

    for side, d in hops:
        if d >= fs - 2 and side == 0:
            for s in order[1:] if d == fs - 1 else order[:1]:
                send("up_z", s, up_piece(ahead(s), g), wup.at[i, g], slice_of(s))
        take_relay("out_z", side, d, out_block, out_cross)
    arrive("mixed", 0, mixw.at[jy], across)
    send("mixed", 2, mixw.at[jy], mixw.at[jy], core)
    arrive("mixed", 1, mixw.at[jc], core)
    arrive("mixed", 2, mixw.at[jd], core)
    for made in local:
        made.wait()

    def whole(ref, k):
        return ref[k].reshape(2 * half, width)

    for side, d in hops:
        has = i >= d if side == 0 else i + d < fs
        b = i - d if side == 0 else i + d

        @pl.when(has)
        def _():
            arrive("out_x", hop(side, d), wo.at[b, 1 - g], twin)

    total = stream_ref[...].astype(f32)
    for k in range(fs):
        total += jnp.dot(mixw[k], whole(wo, k), preferred_element_type=f32)
    rows[j, i] = total.astype(bf16)

    start_relay("rows_z", rows.at[j, i], rows.at[j, i])
    send("rows_y", 0, rows.at[j, i], rows.at[j, i], across)
    send("rows_c", 0, rows.at[j, i], rows.at[j, i], core)

    for s in order:
        b = behind(s)
        arrive("up_z", s, wup.at[b, g], slice_of(s))
        send("up_x", s, wup.at[b, g], wup.at[b, g], twin)
    arrive("rows_y", 0, rows.at[jy, i], across)
    send("rows_d", 0, rows.at[jy, i], rows.at[jy, i], core)

    def rows_block(b):
        return rows.at[j, b]

    def rows_cross(b, n, has):
        send("rows_y", n + 1, rows_block(b), rows_block(b), across, has)
        send("rows_c", n + 1, rows_block(b), rows_block(b), core, has)

    for side, d in hops:
        if d >= fs - 2 and side == 0:
            for s in order[1:] if d == fs - 1 else order[:1]:
                send("down_z", s, down_piece(ahead(s), g), wdn.at[i, g], slice_of(s))
        take_relay("rows_z", side, d, rows_block, rows_cross)
    arrive("gain", 0, gains.at[jy], across)
    arrive("gain", 1, gains.at[jc], core)
    arrive("gain", 2, gains.at[jd], diag)
    for s in order:
        arrive("up_x", s, wup.at[behind(s), 1 - g], twin)

    def hidden(t):
        wide = [rows[k, t].astype(f32) for k in range(rows.shape[0])]
        energy = sum(jnp.sum(w * w, axis=1, keepdims=True) for w in wide)
        scale = lax.rsqrt(energy * (1.0 / (len(wide) * width)) + epsilon)
        up = None
        for k, w in enumerate(wide):
            normed = (w * scale * gains[k].astype(f32)).astype(bf16)
            term = jnp.dot(normed, whole(wup, k), preferred_element_type=f32)
            up = term if up is None else up + term
        return jnp.square(jnp.maximum(up, 0.0)).astype(bf16)

    def cross_down(s):
        arrive("down_z", s, wdn.at[behind(s), g], slice_of(s))
        send("down_x", s, wdn.at[behind(s), g], wdn.at[behind(s), g], twin)

    arrive("rows_c", 0, rows.at[jc, i], core)
    arrive("rows_d", 0, rows.at[jd, i], core)
    acts[i] = hidden(i)
    for side, d in hops:
        has = i >= d if side == 0 else i + d < fs
        b = i - d if side == 0 else i + d
        n = hop(side, d) + 1
        if d == fs - 1 and side == 0:
            cross_down(order[0])

        @pl.when(has)
        def _():
            arrive("rows_y", n, rows.at[jy, b], across)
            send("rows_d", n, rows.at[jy, b], rows.at[jy, b], core, lambda has=has: has)
            arrive("rows_c", n, rows.at[jc, b], core)
            arrive("rows_d", n, rows.at[jd, b], core)
            acts[b] = hidden(b)

    last = order + [0]

    def column(n, k):
        ck, yk = k % 2, k // 2
        w = whole(wdn, k)

        @pl.when(ck != c)
        def _():
            for s in last:
                t = ahead(s)
                send_c[yk, t] = jnp.dot(acts[t], w, preferred_element_type=f32).astype(bf16)
                send("sum_c", n * fs + s, send_c.at[yk, t], got_c.at[yk, t], core, lambda: ck != c)

        @pl.when(ck == c)
        def _():
            for s in last:
                t = ahead(s)
                part = jnp.dot(acts[t], w, preferred_element_type=f32)
                arrive("sum_c", n * fs + s, got_c.at[yk, t], core)
                kept[t] = part + got_c[yk, t].astype(f32)

                @pl.when(yk != y)
                def _():
                    send_y[t] = kept[t].astype(bf16)
                    send("sum_y", s, send_y.at[t], got_y.at[t], across, lambda: both(ck == c, yk != y))

                @pl.when(yk == y)
                def _():
                    mine[t] = kept[t]

    def owned(given):
        @pl.when(given)
        def _():
            for s in order:
                t = ahead(s)
                arrive("sum_y", s, got_y.at[t], across)
                send_z[t] = (mine[t] + got_y[t].astype(f32)).astype(bf16)
                send("sum_z", s, send_z.at[t], got_z.at[i], slice_of(s), lambda: given)

    early = jnp.logical_or(behind(0) == j, behind(order[0]) == j)
    for n, s in enumerate([0] + order):
        if 0 < n < len(order):
            cross_down(order[n])
        if s > 0:
            arrive("down_x", s, wdn.at[behind(s), 1 - g], twin)
        column(n, behind(s))
        if n == len(order) - 1:
            owned(early)
    owned(jnp.logical_not(early))
    arrive("sum_y", 0, got_y.at[i], across)
    branch = mine[i] + got_y[i].astype(f32)
    for s in order:
        b = behind(s)
        arrive("sum_z", s, got_z.at[b], slice_of(s))
        branch += got_z[b].astype(f32)
    result_ref[...] = (rows[j, i].astype(f32) + branch).astype(bf16)
    for made, given in sent:
        if given is None:
            made.wait_send()
        else:
            block = wo.at[0, 0] if made[0].startswith("out") else rows.at[0, 0]
            pl.when(given())(copy(*made, block, block, core).wait_send)


def kernel_body(fs, tp, stream, mixed, out_weight, norm_gain, up_weight, down_weight):
    tokens, width = stream.shape
    half = out_weight.shape[0] // 2
    slots, count = slot_table(fs)
    vmem, anywhere = pl.BlockSpec(memory_space=pltpu.VMEM), pl.BlockSpec(memory_space=pl.ANY)
    weights = pltpu.VMEM((fs, 2, half, width), jnp.bfloat16)
    blocks = pltpu.VMEM((fs, tokens, width), jnp.bfloat16)
    columns = pltpu.VMEM((2, fs, tokens, width), jnp.bfloat16)
    sums = pltpu.VMEM((fs, tokens, width), jnp.float32)
    return pl.pallas_call(
        functools.partial(layer_kernel, fs, slots),
        out_shape=jax.ShapeDtypeStruct((tokens, width), jnp.bfloat16),
        in_specs=[vmem, vmem, anywhere, vmem, anywhere, anywhere],
        out_specs=vmem,
        scratch_shapes=[
            pltpu.VMEM((tp, tokens, width), jnp.bfloat16),
            pltpu.VMEM((tp, 1, width), jnp.bfloat16),
            weights, weights, weights,
            pltpu.VMEM((tp, fs, tokens, width), jnp.bfloat16),
            blocks,
            sums, sums,
            columns, columns, blocks, blocks, blocks, blocks,
            pltpu.SemaphoreType.DMA((count,)),
            pltpu.SemaphoreType.DMA((count,)),
            pltpu.SemaphoreType.DMA((8,)),
        ],
        compiler_params=pltpu.CompilerParams(
            collective_id=0, has_side_effects=True, vmem_limit_bytes=56 * 1024 * 1024
        ),
    )(stream, mixed, out_weight, norm_gain.reshape(1, width), up_weight, down_weight)


def solution(mesh):
    placed = (
        P(("grp", "fs"), "tp"),
        P(("grp", "fs"), "tp"),
        P("fs", "tp"),
        P("tp"),
        P("fs", "tp"),
        P("tp", "fs"),
    )
    fs, tp = mesh.shape["fs"], mesh.shape["tp"]

    def call(stream, mixed, out_weight, norm_gain, up_weight, down_weight):
        width, hidden = up_weight.shape
        tokens = stream.shape[0] // mesh.shape["grp"]
        moved_weights = 2 * width * hidden // tp
        moved_rows = 2 * tokens * width + 2 * width * hidden // (tp * fs)
        aligned = fs == tp == 4 and (width // tp) % 256 == 0 and (tokens // fs) % 16 == 0
        aligned = aligned and hidden == tp * width
        body = spread_body if moved_rows < moved_weights else gathered_body
        if aligned and moved_rows < moved_weights:
            body = functools.partial(kernel_body, fs, tp)
        return sharded(body)(stream, mixed, out_weight, norm_gain, up_weight, down_weight)

    def sharded(body):
        return jax.shard_map(
            body, mesh=mesh, in_specs=placed, out_specs=P(("grp", "fs"), "tp"), check_vma=False
        )

    return call
```
